32 devices in a mesh: sp: 4 (over y, x), tp: 8 (over z, core).
Axes of the slice: x: 2, y: 2, z: 4, core: 2. Of those that a mesh axis runs over, the one named last changes fastest.
Arguments:
- queries: bfloat16 [2048, 1536], P('sp', 'tp'), may hold values from -34 to 34
- latent: bfloat16 [2048, 512], P('sp'), may hold values from -6 to 6
- rot_key: bfloat16 [2048, 32], P('sp'), may hold values from -34 to 34
- latent_gain: float32 [512], replicated, may hold values from 0.1 to 1.9
- key_up: bfloat16 [512, 1024], P(None, 'tp'), may hold values from -0.25 to 0.25
- value_up: bfloat16 [512, 1024], P(None, 'tp'), may hold values from -0.70710678 to 0.70710678
- query_gain: float32 [96], replicated, may hold values from 0.5 to 6
- key_gain: float32 [96], replicated, may hold values from 0.5 to 6
- out_gain: float32 [1024], replicated, may hold values from 0.1 to 1.9
- out_weight: bfloat16 [1024, 2048], replicated, may hold values from -0.1875 to 0.1875
- residual: bfloat16 [2048, 2048], P(('sp', 'tp')), may hold values from -6 to 6
- ffn_gain: float32 [2048], replicated, may hold values from 0.1 to 1.9
- routes: int32 [2048, 2], P(('sp', 'tp')), may hold values from 0 to 3, all different within a row; in each aligned block of 64 rows (0 to 63, 64 to 127, ...) at most 36 rows name the same one
- route_weights: float32 [2048, 2], P(('sp', 'tp')), may hold values from 0.2 to 1
- expert_gate: bfloat16 [4, 2048, 2048], P('sp', None, 'tp'), may hold values from -0.125 to 0.125
- expert_up: bfloat16 [4, 2048, 2048], P('sp', None, 'tp'), may hold values from -0.125 to 0.125
- expert_down: bfloat16 [4, 2048, 2048], P('sp', 'tp'), may hold values from -0.125 to 0.125
Outputs:
- layer_out: bfloat16 [2048, 2048], P(('sp', 'tp'))
The draws below stay inside these ranges and needn't reach their ends.
Inputs may be any that keep to these rules, and one draw needn't show every extreme that they name: `routes`: the 2 experts of a token differ. Among the 64 rows of one device each expert is named by at most 36 rows, a bound that some block reaches.
All inputs are finite; a program needn't handle non-finite values.
Results may differ from the reference program's by a relative error of at most 0.02.
The reference program's roundings to bfloat16 on the way count: a program that leaves them out, or rounds other values in their place, can miss the bound.
Values may be sent and summed in bfloat16 or wider, within the bound.
A program may use at most 128 MiB of HBM per device.

```python
import math
import jax
import jax.numpy as jnp
import numpy as np
from jax import lax

D = 2048
HEADS = 16
NOPE = 64
ROPE = 32
VH = 64
LAT = 512
FF_E = 2048
TOPK = 2
TOK_DEV = 64
QK = 96
ATT_WIDTH = 1024
POS_SP = 512
LENGTH = 2048
EXPERTS = 4
CAP = 36
N_SP = 4
N_TP = 8


def drawn_pair(key):
    base_query = jnp.clip(jax.random.normal(jax.random.fold_in(key, 11), (LENGTH, HEADS, QK), jnp.float32), -6.0, 6.0)
    base_key = jnp.clip(jax.random.normal(jax.random.fold_in(key, 12), (LENGTH, ROPE), jnp.float32), -6.0, 6.0)
    return (base_query.reshape(LENGTH, HEADS * QK), base_key)


def draw_queries(key, part):
    return drawn_pair(key)[0].astype(jnp.bfloat16)


def draw_rot_key(key, part):
    return drawn_pair(key)[1].astype(jnp.bfloat16)


def head_gains(key):
    spread = 1.0 + 0.18 * jax.random.uniform(jax.random.fold_in(key, 1), (QK,), jnp.float32, -2.5, 2.5)
    return spread


def draw_query_gain(key, part):
    return head_gains(jax.random.fold_in(key, 21))


def draw_key_gain(key, part):
    return head_gains(jax.random.fold_in(key, 22))


def draw_value_up(key, part):
    head_ids = jnp.arange(HEADS * VH, dtype=jnp.int32) // VH
    rising = head_ids.astype(jnp.float32) / max(HEADS - 1, 1)
    entries = jnp.clip(jax.random.normal(jax.random.fold_in(key, 32), (LAT, HEADS * VH), jnp.float32), -4.0, 4.0)
    column_scale = 3.0 ** rising
    return (entries * column_scale[None, :] / jnp.sqrt(jnp.float32(LAT))).astype(jnp.bfloat16)


def shard_levels(rng, extent, shards, smallest, top_value):
    loudness = 1.0
    for position, parts in shards:
        steps = jax.random.uniform(jax.random.fold_in(jax.random.fold_in(rng, 6), position), (parts,), jnp.float32, smallest / len(shards), top_value / len(shards))
        loudness = loudness * jnp.repeat(jnp.exp(steps), extent[position] // parts).reshape((-1,) + (1,) * (len(extent) - 1 - position))
    return loudness


def shared_out(own_key, own, number, rows, number_of, top, reach, lean):
    ranking = jax.random.permutation(own_key, number_of)
    packed, ordinary = load_shares(number_of, rows * top, reach, lean, True), load_shares(number_of, rows * top, reach, lean, False)
    places = jnp.arange(number_of)

    def named(lengths, offset_by):
        used = int((lengths > 0).sum())
        fixed = max(1, used // 4)
        moved = fixed + (places - fixed + offset_by * (used - fixed)) % max(1, number_of - fixed)
        return jnp.zeros((number_of,), jnp.int32).at[ranking[jnp.where(places < fixed, places, moved)]].set(jnp.asarray(lengths, jnp.int32))

    lengths = jnp.where(number % 4 == 0, named(packed, number // 4), named(ordinary, number - number // 4 - 1))
    mixed = jax.random.permutation(jax.random.fold_in(own, 3), number_of)
    giver, sink = mixed[0:number_of // 2 * 2:2], mixed[1:number_of // 2 * 2:2]
    slack = jnp.minimum(lengths[giver] - 1, reach - lengths[sink]) // 2
    slack = jnp.where((giver == ranking[0]) | (sink == ranking[0]) | (lengths[sink] == 0), 0, jnp.maximum(slack, 0))
    moved = jax.random.randint(jax.random.fold_in(own, 4), (number_of // 2,), 0, 1 << 20) % (slack + 1)
    lengths = lengths.at[giver].add(-moved).at[sink].add(moved)
    members = jnp.searchsorted(jnp.cumsum(lengths), jnp.arange(rows * top), side="right").astype(jnp.int32)
    listing = members.reshape(top, rows).T
    listing = listing[jax.random.permutation(jax.random.fold_in(own, 1), rows)]
    offset_by = jax.random.randint(jax.random.fold_in(own, 2), (rows, 1), 0, top)
    return jnp.take_along_axis(listing, (jnp.arange(top)[None, :] + offset_by) % top, axis=1)


def load_shares(number_of, total, bound, slope, full):
    portions = [(1 << 20) // math.isqrt(rank ** slope) + 1 for rank in range(1, number_of + 1)]
    largest = bound if full else min(bound, max(-(-total // number_of), total * portions[0] // sum(portions)))
    least = 1 if total - largest >= number_of - 1 else 0
    given, rest = [largest] + [least] * (number_of - 1), total - largest - least * (number_of - 1)
    while rest > 0:
        candidates = [i for i in range(1, number_of) if given[i] < largest] or [i for i in range(1, number_of) if given[i] < bound]
        pool, budget = sum([portions[i] for i in candidates]), rest
        for i in candidates:
            more = min(bound - given[i], max(1, budget * portions[i] // pool), rest)
            given[i] = given[i] + more
            rest = rest - more
    return np.array(given)


def bell_draw(rng, dims, deviation, bound, split=(), kind=jnp.bfloat16):
    values = deviation * jax.random.normal(rng, dims, jnp.float32)
    if split:
        values = values * shard_levels(rng, dims, split, -0.22, 0.18)
    return jnp.clip(values, -bound, bound).astype(kind)


def setup_inputs(seed: int = 0) -> dict:
    streams_of = jax.random.split(jax.random.key(seed), 18)
    queries = draw_queries(jax.random.fold_in(streams_of[17], 71), 0)
    latent = bell_draw(streams_of[1], (LENGTH, LAT), 1.0, 6.0, ((0, 4),))
    rot_key = draw_rot_key(jax.random.fold_in(streams_of[17], 71), 0)
    latent_gain = jnp.clip(1.0 + 0.18 * jax.random.normal(streams_of[3], (LAT,), jnp.float32), 0.1, 1.9)
    key_up = bell_draw(streams_of[4], (LAT, HEADS * NOPE), LAT ** -0.5, 0.25, ((1, 8),))
    value_up = draw_value_up(jax.random.fold_in(streams_of[17], 71), 0)
    query_gain = draw_query_gain(jax.random.fold_in(streams_of[17], 71), 0)
    key_gain = draw_key_gain(jax.random.fold_in(streams_of[17], 71), 0)
    out_gain = jnp.clip(1.0 + 0.18 * jax.random.normal(streams_of[8], (ATT_WIDTH,), jnp.float32), 0.1, 1.9)
    out_weight = bell_draw(streams_of[9], (ATT_WIDTH, D), ATT_WIDTH ** -0.5, 0.1875)
    residual = bell_draw(streams_of[10], (LENGTH, D), 1.0, 6.0, ((0, 32),))
    ffn_gain = jnp.clip(1.0 + 0.18 * jax.random.normal(streams_of[11], (D,), jnp.float32), 0.1, 1.9)
    routes_keys = jax.random.split(jax.random.fold_in(streams_of[12], 1), LENGTH // TOK_DEV)
    routes_turns = jax.random.permutation(jax.random.fold_in(streams_of[12], 3), LENGTH // TOK_DEV)
    routes = jax.vmap(lambda own, number: shared_out(jax.random.fold_in(streams_of[12], 2), own, number, TOK_DEV, EXPERTS, TOPK, CAP, 1))(routes_keys, routes_turns).reshape((LENGTH, TOPK))
    route_weights = jnp.clip(0.2 + 0.8 * jax.random.uniform(streams_of[13], (LENGTH, TOPK), jnp.float32) ** shard_levels(streams_of[13], (LENGTH, TOPK), ((0, 32),), -0.2, 0.2), 0.2, 1.0)
    expert_gate = bell_draw(streams_of[14], (EXPERTS, D, FF_E), D ** -0.5, 0.125, ((0, 4), (2, 8)))
    expert_up = bell_draw(streams_of[15], (EXPERTS, D, FF_E), D ** -0.5, 0.125, ((0, 4), (2, 8)))
    expert_down = bell_draw(streams_of[16], (EXPERTS, FF_E, D), FF_E ** -0.5, 0.125, ((0, 4), (1, 8)))
    return dict(queries=queries, latent=latent, rot_key=rot_key, latent_gain=latent_gain, key_up=key_up, value_up=value_up, query_gain=query_gain, key_gain=key_gain, out_gain=out_gain, out_weight=out_weight, residual=residual, ffn_gain=ffn_gain, routes=routes, route_weights=route_weights, expert_gate=expert_gate, expert_up=expert_up, expert_down=expert_down)


epsilon = 1e-06
rope_base = 10000.0

def rms_scale(values):
    return lax.rsqrt(lax.optimization_barrier(jnp.mean(values * values, axis=-1, keepdims=True)) + epsilon)

def rotate_half(values, angles):
    half_dims = values.shape[-1] // 2
    first_half = values[..., :half_dims]
    second_half = values[..., half_dims:]
    cosine = jnp.cos(angles)
    sine_val = jnp.sin(angles)
    return jnp.concatenate([first_half * cosine - second_half * sine_val, second_half * cosine + first_half * sine_val], axis=-1)

def head_prepare(raw_rows, gain_vec, angles):
    normed_rows = raw_rows * rms_scale(raw_rows) * gain_vec
    turned_rows = rotate_half(normed_rows[..., NOPE:], angles[:, None, :])
    return jnp.concatenate([normed_rows[..., :NOPE], turned_rows], axis=-1).astype(jnp.bfloat16)

def attend_head(head_inputs):
    query_head, key_head, value_head = head_inputs
    query_f32 = query_head.astype(jnp.float32)
    key_f32 = key_head.astype(jnp.float32)
    value_f32 = value_head.astype(jnp.float32)
    block_count = LENGTH // POS_SP
    query_blocks = query_f32.reshape(block_count, POS_SP, QK)
    key_pos = jnp.arange(LENGTH, dtype=jnp.int32)

    def one_block(block_inputs):
        block_index, query_block = block_inputs
        scores = jnp.dot(query_block, key_f32.T, precision=lax.Precision.HIGHEST) * QK ** (-0.5)
        query_pos = block_index * POS_SP + jnp.arange(POS_SP, dtype=jnp.int32)
        allowed = key_pos[None, :] <= query_pos[:, None]
        scores = jnp.where(allowed, scores, -1e+30)
        row_peak = lax.optimization_barrier(jnp.max(scores, axis=1, keepdims=True))
        exponent = jnp.where(allowed, jnp.exp(scores - row_peak), 0.0)
        row_total = lax.optimization_barrier(jnp.sum(exponent, axis=1))
        rounded_exp = lax.optimization_barrier(exponent.astype(jnp.bfloat16)).astype(jnp.float32)
        result = jnp.dot(rounded_exp, value_f32, precision=lax.Precision.HIGHEST) / row_total[:, None]
        return result.astype(jnp.bfloat16)
    outputs = lax.map(one_block, (jnp.arange(block_count, dtype=jnp.int32), query_blocks))
    return outputs.reshape(LENGTH, VH)

def reference(queries, latent, rot_key, latent_gain, key_up, value_up, query_gain, key_gain, out_gain, out_weight, residual, ffn_gain, routes, route_weights, expert_gate, expert_up, expert_down):
    lat_f32 = latent.astype(jnp.float32)
    normed_latent = (lat_f32 * rms_scale(lat_f32) * latent_gain).astype(jnp.bfloat16)
    key_nope = jnp.dot(normed_latent, key_up, preferred_element_type=jnp.float32).astype(jnp.bfloat16)
    values = jnp.dot(normed_latent, value_up, preferred_element_type=jnp.float32).astype(jnp.bfloat16)
    positions = jnp.arange(LENGTH, dtype=jnp.int32)
    inverse = rope_base ** (-jnp.arange(0, ROPE, 2, dtype=jnp.float32) / ROPE)
    angles = positions.astype(jnp.float32)[:, None] * inverse[None, :]
    shared = jnp.broadcast_to(rot_key.astype(jnp.float32)[:, None, :], (LENGTH, HEADS, ROPE))
    raw_keys = jnp.concatenate([key_nope.astype(jnp.float32).reshape(LENGTH, HEADS, NOPE), shared], axis=-1)
    key_rows = head_prepare(raw_keys, key_gain, angles)
    query_rows = head_prepare(queries.astype(jnp.float32).reshape(LENGTH, HEADS, QK), query_gain, angles)
    value_heads = values.reshape(LENGTH, HEADS, VH)
    attended = lax.map(attend_head, (jnp.transpose(query_rows, (1, 0, 2)), jnp.transpose(key_rows, (1, 0, 2)), jnp.transpose(value_heads, (1, 0, 2))))
    att_rows = jnp.transpose(attended, (1, 0, 2)).reshape(LENGTH, ATT_WIDTH).astype(jnp.float32)
    normed_att = (att_rows * rms_scale(att_rows) * out_gain).astype(jnp.bfloat16)
    group_width = ATT_WIDTH // N_TP
    mixed = jnp.zeros((LENGTH, D), jnp.float32)
    for group_index in range(N_TP):
        low = group_index * group_width
        partial_value = jnp.dot(normed_att[:, low:low + group_width], out_weight[low:low + group_width], preferred_element_type=jnp.float32).astype(jnp.bfloat16)
        mixed = mixed + lax.optimization_barrier(partial_value).astype(jnp.float32)
    middle = residual.astype(jnp.float32) + mixed
    ffn_input = (middle * rms_scale(middle) * ffn_gain).astype(jnp.bfloat16)
    flat_routes = routes.reshape(-1).astype(jnp.int32)
    row_order = jnp.argsort(flat_routes, stable=True).astype(jnp.int32)
    expert_counts = lax.optimization_barrier(jnp.sum((flat_routes[:, None] == jnp.arange(EXPERTS, dtype=jnp.int32)[None, :]).astype(jnp.int32), axis=0))
    offsets = (jnp.cumsum(expert_counts) - expert_counts).astype(jnp.int32)
    row_limit = N_SP * N_TP * CAP
    weights_flat = route_weights.reshape(-1).astype(jnp.float32)
    hidden_width = FF_E // N_TP

    def per_expert(expert_id, combined):
        slot_ids = jnp.arange(row_limit, dtype=jnp.int32)
        is_live = slot_ids < expert_counts[expert_id]
        picked = row_order[jnp.minimum(offsets[expert_id] + slot_ids, LENGTH * TOPK - 1)]
        token_ids = (picked // TOPK).astype(jnp.int32)
        expert_in = ffn_input[token_ids]
        gate_pre = jnp.dot(expert_in, expert_gate[expert_id], preferred_element_type=jnp.float32)
        up_pre = jnp.dot(expert_in, expert_up[expert_id], preferred_element_type=jnp.float32)
        hidden = (jax.nn.silu(gate_pre) * up_pre).astype(jnp.bfloat16)
        down_weight = expert_down[expert_id]
        down_sum = jnp.zeros((row_limit, D), jnp.float32)
        for group_index in range(N_TP):
            low = group_index * hidden_width
            partial_value = jnp.dot(hidden[:, low:low + hidden_width], down_weight[low:low + hidden_width], preferred_element_type=jnp.float32).astype(jnp.bfloat16)
            down_sum = down_sum + lax.optimization_barrier(partial_value).astype(jnp.float32)
        expert_out = lax.optimization_barrier(down_sum.astype(jnp.bfloat16)).astype(jnp.float32)
        contrib_rows = expert_out * (weights_flat[picked] * is_live.astype(jnp.float32))[:, None]
        return combined.at[token_ids].add(contrib_rows)
    combined = lax.fori_loop(0, EXPERTS, per_expert, jnp.zeros((LENGTH, D), jnp.float32))
    return (middle + combined).astype(jnp.bfloat16)
```

```python
import functools

import jax
import jax.numpy as jnp
from jax import lax
from jax.experimental import pallas as pl
from jax.experimental.pallas import tpu as pltpu
from jax.sharding import PartitionSpec as P

D = 2048
NOPE = 64
ROPE = 32
VH = 64
TOPK = 2
QK = 96

epsilon = 1e-06
rope_base = 10000.0
MESH_ID = pl.DeviceIdType.MESH


class Place:
    def __init__(self, n_sp, n_z):
        self.n_sp, self.n_z = n_sp, n_z
        self.sp = lax.axis_index("sp")
        self.tp = lax.axis_index("tp")
        self.core = lax.rem(self.tp, 2)
        self.z = lax.div(self.tp, 2)

    def partner(self):
        return (self.sp, self.tp + 1 - 2 * self.core)

    def sp_peer(self, step):
        return lax.rem(self.sp + step, self.n_sp)

    def z_peer(self, step):
        return lax.rem(self.z + step, self.n_z)

    def sp_id(self, index):
        return (index, self.tp)

    def z_id(self, index):
        return (self.sp, 2 * index + self.core)

    def barrier(self, use_sp, use_z):
        sem = pltpu.get_barrier_semaphore()
        count = 1
        pl.semaphore_signal(sem, inc=1, device_id=self.partner(), device_id_type=MESH_ID)
        if use_sp:
            for step in range(1, self.n_sp):
                pl.semaphore_signal(
                    sem, inc=1, device_id=self.sp_id(self.sp_peer(step)), device_id_type=MESH_ID
                )
            count += self.n_sp - 1
        if use_z:
            for step in range(1, self.n_z):
                pl.semaphore_signal(
                    sem, inc=1, device_id=self.z_id(self.z_peer(step)), device_id_type=MESH_ID
                )
            count += self.n_z - 1
        pl.semaphore_wait(sem, count)


def remote(src, dst, send, recv, device):
    return pltpu.make_async_remote_copy(
        src_ref=src,
        dst_ref=dst,
        send_sem=send,
        recv_sem=recv,
        device_id=device,
        device_id_type=MESH_ID,
    )


class GroupMove:
    def __init__(self, place, axis, scatter, x_ref, o_ref, sems):
        self.place, self.axis, self.scatter = place, axis, scatter
        self.x_ref, self.o_ref = x_ref, o_ref
        self.local_sem, self.ss, self.rs, self.ps, self.pr = sems
        self.count = place.n_sp if axis == "sp" else place.n_z
        self.me = place.sp if axis == "sp" else place.z

    def start(self):
        p, core = self.place, self.place.core
        peer, to_id = (p.sp_peer, p.sp_id) if self.axis == "sp" else (p.z_peer, p.z_id)
        own = self.x_ref.at[self.me] if self.scatter else self.x_ref
        self.copies = []
        for step in range(1, self.count):
            dst = peer(step)
            src = self.x_ref.at[dst] if self.scatter else self.x_ref
            copy = remote(
                src,
                self.o_ref.at[core, self.me],
                self.ss.at[step],
                self.rs.at[step],
                to_id(dst),
            )
            copy.start()
            self.copies.append(copy)
        self.local = pltpu.make_async_copy(own, self.o_ref.at[core, self.me], self.local_sem.at[0])
        self.local.start()
        self.relays = [
            remote(
                own, self.o_ref.at[core, self.me], self.ps.at[0], self.pr.at[0], p.partner()
            )
        ]
        self.relays[0].start()

    def relay(self):
        core = self.place.core
        for step in range(1, self.count):
            src = lax.rem(self.me - step + self.count, self.count)
            self.copies[step - 1].wait_recv()
            block = self.o_ref.at[core, src]
            copy = remote(block, block, self.ps.at[step], self.pr.at[step], self.place.partner())
            copy.start()
            self.relays.append(copy)

    def finish(self):
        for copy in self.copies:
            copy.wait_send()
        for copy in self.relays:
            copy.wait()
        self.local.wait()


def move_sems(count):
    return [pltpu.SemaphoreType.DMA((1,))] + [pltpu.SemaphoreType.DMA((count,))] * 4


def vmem():
    return pl.BlockSpec(memory_space=pltpu.VMEM)


def group_move(x, axis, scatter, n_sp, n_z, collective_id, name):
    count = n_sp if axis == "sp" else n_z
    block = x.shape[1:] if scatter else x.shape

    def kernel(x_ref, o_ref, *sems):
        place = Place(n_sp, n_z)
        place.barrier(axis == "sp", axis == "z")
        move = GroupMove(place, axis, scatter, x_ref, o_ref, sems)
        move.start()
        move.relay()
        move.finish()

    return pl.pallas_call(
        kernel,
        out_shape=jax.ShapeDtypeStruct((2, count) + block, x.dtype),
        in_specs=[vmem()],
        out_specs=vmem(),
        scratch_shapes=move_sems(count),
        compiler_params=pltpu.CompilerParams(
            collective_id=collective_id, has_side_effects=True, vmem_limit_bytes=60 << 20
        ),
        name=name,
    )(x)


def first_exchange(bundle, residual, meta, n_sp, n_z):
    def kernel(kv_ref, res_ref, meta_ref, kv_out, res_out, meta_out, kv_local, kv_s, kv_r, *sems):
        place = Place(n_sp, n_z)
        place.barrier(True, True)
        copies = []
        for step in range(1, n_sp):
            copy = remote(
                kv_ref,
                kv_out.at[place.sp],
                kv_s.at[step],
                kv_r.at[step],
                place.sp_id(place.sp_peer(step)),
            )
            copy.start()
            copies.append(copy)
        local = pltpu.make_async_copy(kv_ref, kv_out.at[place.sp], kv_local.at[0])
        local.start()
        meta_move = GroupMove(place, "z", False, meta_ref, meta_out, sems[:5])
        res_move = GroupMove(place, "z", False, res_ref, res_out, sems[5:])
        meta_move.start()
        res_move.start()
        meta_move.relay()
        res_move.relay()
        for copy in copies:
            copy.wait()
        local.wait()
        meta_move.finish()
        res_move.finish()

    return pl.pallas_call(
        kernel,
        out_shape=(
            jax.ShapeDtypeStruct((n_sp,) + bundle.shape, bundle.dtype),
            jax.ShapeDtypeStruct((2, n_z) + residual.shape, residual.dtype),
            jax.ShapeDtypeStruct((2, n_z) + meta.shape, meta.dtype),
        ),
        in_specs=[vmem()] * 3,
        out_specs=(vmem(),) * 3,
        scratch_shapes=[
            pltpu.SemaphoreType.DMA((1,)),
            pltpu.SemaphoreType.DMA((n_sp,)),
            pltpu.SemaphoreType.DMA((n_sp,)),
        ]
        + move_sems(n_z) * 2,
        compiler_params=pltpu.CompilerParams(
            collective_id=0, has_side_effects=True, vmem_limit_bytes=60 << 20
        ),
        name="first_exchange",
    )(bundle, residual, meta)


CHUNKS = 4


def return_rows(partial, mixer, middle, n_sp, n_z):
    rows = partial.shape[2]
    tok = middle.shape[0]
    width = D // CHUNKS

    def kernel(y_ref, mix_ref, mid_ref, o_ref, pbuf, sbuf, rbuf, cbuf, fbuf, *sems):
        pair_s, pair_r, sp_s, sp_r, z_s, z_r = sems
        place = Place(n_sp, n_z)
        core = place.core
        place.barrier(True, True)
        pairs, sends, zsends = {}, {}, {}
        order = list(range(1, n_sp)) + [0]
        for q in range(CHUNKS):
            cols = pl.ds(q * width, width)
            for step in order:
                dst = place.sp_peer(step)
                copy = remote(
                    y_ref.at[1 - core, dst, :, cols],
                    pbuf.at[dst, :, cols],
                    pair_s.at[q, step],
                    pair_r.at[q, step],
                    place.partner(),
                )
                copy.start()
                pairs[q, step] = copy
        for q in range(CHUNKS):
            cols = pl.ds(q * width, width)
            for step in order:
                dst = place.sp_peer(step)
                pairs[q, step].wait_recv()
                total = (
                    y_ref[core, dst, :, cols].astype(jnp.float32)
                    + pbuf[dst, :, cols].astype(jnp.float32)
                ).astype(jnp.bfloat16)
                if step == 0:
                    rbuf[dst, :, cols] = total
                else:
                    sbuf[dst, :, cols] = total
                    copy = remote(
                        sbuf.at[dst, :, cols],
                        rbuf.at[place.sp, :, cols],
                        sp_s.at[q, step],
                        sp_r.at[q, step],
                        place.sp_id(dst),
                    )
                    copy.start()
                    sends[q, step] = copy
        for q in range(CHUNKS):
            cols = pl.ds(q * width, width)
            for step in range(1, n_sp):
                sends[q, step].wait_recv()
            combined = jnp.zeros((n_z * tok, width), jnp.float32)
            for src in range(n_sp):
                combined += jnp.dot(
                    mix_ref[src], rbuf[src, :, cols], preferred_element_type=jnp.float32
                )
            cbuf[:, :, cols] = combined.astype(jnp.bfloat16).reshape(n_z, tok, width)
            for step in range(1, n_z):
                dst = place.z_peer(step)
                copy = remote(
                    cbuf.at[dst, :, cols],
                    fbuf.at[place.z, :, cols],
                    z_s.at[q, step],
                    z_r.at[q, step],
                    place.z_id(dst),
                )
                copy.start()
                zsends[q, step] = copy
        for q in range(CHUNKS):
            cols = pl.ds(q * width, width)
            total = mid_ref[:, cols] + cbuf[place.z, :, cols].astype(jnp.float32)
            for step in range(1, n_z):
                src = lax.rem(place.z - step + n_z, n_z)
                zsends[q, step].wait_recv()
                total += fbuf[src, :, cols].astype(jnp.float32)
            o_ref[:, cols] = total.astype(jnp.bfloat16)
        for group in (pairs, sends, zsends):
            for copy in group.values():
                copy.wait_send()

    dma = pltpu.SemaphoreType.DMA
    block = pltpu.VMEM((n_sp, rows, D), jnp.bfloat16)
    zblock = pltpu.VMEM((n_z, tok, D), jnp.bfloat16)
    return pl.pallas_call(
        kernel,
        out_shape=jax.ShapeDtypeStruct((tok, D), jnp.bfloat16),
        in_specs=[vmem()] * 3,
        out_specs=vmem(),
        scratch_shapes=[block, block, block, zblock, zblock]
        + [dma((CHUNKS, n_sp))] * 4
        + [dma((CHUNKS, n_z))] * 2,
        compiler_params=pltpu.CompilerParams(
            collective_id=3, has_side_effects=True, vmem_limit_bytes=60 << 20
        ),
        name="return_rows",
    )(partial, mixer, middle)


def rms_scale(values):
    return lax.rsqrt(jnp.mean(values * values, axis=-1, keepdims=True) + epsilon)


def rotate_half(values, angles):
    half_dims = values.shape[-1] // 2
    first_half = values[..., :half_dims]
    second_half = values[..., half_dims:]
    cosine = jnp.cos(angles)
    sine_val = jnp.sin(angles)
    return jnp.concatenate(
        [
            first_half * cosine - second_half * sine_val,
            second_half * cosine + first_half * sine_val,
        ],
        axis=-1,
    )


def head_prepare(raw_rows, gain_vec, angles):
    normed_rows = raw_rows * rms_scale(raw_rows) * gain_vec
    turned_rows = rotate_half(normed_rows[..., NOPE:], angles[:, None, :])
    return jnp.concatenate([normed_rows[..., :NOPE], turned_rows], axis=-1).astype(jnp.bfloat16)


def shards(
    queries,
    latent,
    rot_key,
    latent_gain,
    key_up,
    value_up,
    query_gain,
    key_gain,
    out_gain,
    out_weight,
    residual,
    ffn_gain,
    routes,
    route_weights,
    expert_gate,
    expert_up,
    expert_down,
):
    shard_len = queries.shape[0]
    local_heads = key_up.shape[1] // NOPE
    sp_count = lax.axis_size("sp")
    tp_count = lax.axis_size("tp")
    z_count = tp_count // 2
    tok_count = residual.shape[0]
    my_first = lax.axis_index("sp") * shard_len
    my_last = my_first + shard_len - 1
    positions = my_first + jnp.arange(shard_len, dtype=jnp.int32)
    inverse = rope_base ** (-jnp.arange(0, ROPE, 2, dtype=jnp.float32) / ROPE)
    angles = positions.astype(jnp.float32)[:, None] * inverse[None, :]
    lat_f32 = latent.astype(jnp.float32)
    normed_latent = (lat_f32 * rms_scale(lat_f32) * latent_gain).astype(jnp.bfloat16)
    key_nope = jnp.dot(normed_latent, key_up, preferred_element_type=jnp.float32).astype(
        jnp.bfloat16
    )
    value_rows = jnp.dot(normed_latent, value_up, preferred_element_type=jnp.float32).astype(
        jnp.bfloat16
    )
    shared = jnp.broadcast_to(
        rot_key.astype(jnp.float32)[:, None, :], (shard_len, local_heads, ROPE)
    )
    raw_keys = jnp.concatenate(
        [key_nope.astype(jnp.float32).reshape(shard_len, local_heads, NOPE), shared], axis=-1
    )
    key_rows = head_prepare(raw_keys, key_gain, angles)
    query_rows = head_prepare(
        queries.astype(jnp.float32).reshape(shard_len, local_heads, QK), query_gain, angles
    )
    query_heads = jnp.transpose(query_rows, (1, 0, 2))
    bundle = jnp.concatenate(
        [
            jnp.transpose(key_rows, (1, 2, 0)),
            jnp.transpose(value_rows.reshape(shard_len, local_heads, VH), (1, 2, 0)),
        ],
        axis=1,
    )
    score_scale = QK ** (-0.5)
    init_state = (
        jnp.full((local_heads, shard_len), -1e30, jnp.float32),
        jnp.zeros((local_heads, shard_len), jnp.float32),
        jnp.zeros((local_heads, shard_len, VH), jnp.float32),
    )
    meta = jnp.concatenate(
        [
            routes.astype(jnp.float32),
            route_weights,
            jnp.zeros((tok_count, 128 - 2 * TOPK), jnp.float32),
        ],
        axis=1,
    )
    key_piece, residual_all, meta_all = first_exchange(bundle, residual, meta, sp_count, z_count)
    block_count = sp_count

    def one_block(block_index, running_state):
        first_key = block_index * shard_len

        def compute(inner):
            row_peak, row_total, weighted = inner
            key_part = lax.dynamic_index_in_dim(key_piece, block_index, 0, keepdims=False)
            scores = (
                jnp.einsum(
                    "hqc,hck->hqk",
                    query_heads,
                    key_part[:, :QK, :],
                    preferred_element_type=jnp.float32,
                )
                * score_scale
            )
            key_pos = first_key + jnp.arange(shard_len, dtype=jnp.int32)
            allowed = key_pos[None, None, :] <= positions[None, :, None]
            scores = jnp.where(allowed, scores, -1e30)
            new_peak = jnp.maximum(row_peak, jnp.max(scores, axis=2))
            exponent = jnp.where(allowed, jnp.exp(scores - new_peak[..., None]), 0.0)
            factor = jnp.exp(row_peak - new_peak)
            new_total = row_total * factor + jnp.sum(exponent, axis=2)
            contrib = jnp.einsum(
                "hqk,hvk->hqv",
                exponent.astype(jnp.bfloat16),
                key_part[:, QK:, :],
                preferred_element_type=jnp.float32,
            )
            return (new_peak, new_total, weighted * factor[..., None] + contrib)

        return lax.cond(first_key <= my_last, compute, lambda inner: inner, running_state)

    row_peak, row_total, weighted = lax.fori_loop(0, block_count, one_block, init_state)
    attended = (weighted / row_total[..., None]).astype(jnp.bfloat16)
    head_major = jnp.transpose(attended, (1, 0, 2)).reshape(shard_len, local_heads * VH)
    gathered = group_move(head_major, "z", False, sp_count, z_count, 1, "gather_heads")
    att_rows = (
        jnp.transpose(gathered, (2, 1, 0, 3)).reshape(shard_len, -1).astype(jnp.float32)
    )
    normed_rows = (att_rows * rms_scale(att_rows) * out_gain).astype(jnp.bfloat16)
    mixed = jnp.dot(normed_rows, out_weight, preferred_element_type=jnp.float32)
    residual_rows = jnp.transpose(residual_all, (1, 0, 2, 3)).reshape(shard_len, D)
    middle = residual_rows.astype(jnp.float32) + mixed
    ffn_input = (middle * rms_scale(middle) * ffn_gain).astype(jnp.bfloat16)
    own_middle = lax.dynamic_slice_in_dim(
        middle, lax.axis_index("tp") * tok_count, tok_count, 0
    )
    slot_cap = max(2, 9 * tok_count * TOPK // (8 * sp_count))
    rows = z_count * slot_cap
    core = lax.axis_index("tp") % 2
    part_meta = lax.dynamic_index_in_dim(meta_all, core, 0, keepdims=False)
    part_routes = part_meta[:, :, :TOPK].astype(jnp.int32).reshape(z_count, tok_count * TOPK)
    part_weights = part_meta[:, :, TOPK : 2 * TOPK].reshape(z_count * tok_count, TOPK)
    one_hot = (part_routes[:, :, None] == jnp.arange(sp_count, dtype=jnp.int32)).astype(jnp.int32)
    earlier = jnp.cumsum(one_hot, axis=1) - one_hot
    rank_in = jnp.sum(earlier * one_hot, axis=2)
    slots = rank_in + jnp.arange(z_count, dtype=jnp.int32)[:, None] * slot_cap
    targets = (part_routes * rows + slots).reshape(z_count * tok_count, TOPK)
    hits = targets[:, :, None] == jnp.arange(sp_count * rows, dtype=jnp.int32)
    chooser = jnp.sum(hits.astype(jnp.bfloat16), axis=1)
    mixer = jnp.sum(jnp.where(hits, part_weights[:, :, None], 0.0), axis=1).astype(jnp.bfloat16)
    mixer = jnp.transpose(mixer.reshape(z_count * tok_count, sp_count, rows), (1, 0, 2))
    part_input = lax.dynamic_index_in_dim(
        ffn_input.reshape(z_count, 2, tok_count, D), core, 1, keepdims=False
    ).reshape(z_count * tok_count, D)
    outbound = (
        jnp.einsum("ts,td->sd", chooser, part_input, preferred_element_type=jnp.float32)
        .astype(jnp.bfloat16)
        .reshape(sp_count, rows, D)
    )
    arrived = group_move(outbound, "sp", True, sp_count, z_count, 2, "send_rows")
    row_block = arrived.reshape(2 * sp_count * rows, D)
    gate_pre = jnp.dot(row_block, expert_gate[0], preferred_element_type=jnp.float32)
    up_pre = jnp.dot(row_block, expert_up[0], preferred_element_type=jnp.float32)
    hidden = (jax.nn.silu(gate_pre) * up_pre).astype(jnp.bfloat16)
    served = jnp.dot(hidden, expert_down[0], preferred_element_type=jnp.float32).astype(
        jnp.bfloat16
    )
    return return_rows(
        served.reshape(2, sp_count, rows, D), mixer, own_middle, sp_count, z_count
    )


def solution(mesh):
    return jax.shard_map(
        shards,
        mesh=mesh,
        in_specs=(
            P("sp", "tp"),
            P("sp", None),
            P("sp", None),
            P(),
            P(None, "tp"),
            P(None, "tp"),
            P(),
            P(),
            P(),
            P(),
            P(("sp", "tp"), None),
            P(),
            P(("sp", "tp"), None),
            P(("sp", "tp"), None),
            P("sp", None, "tp"),
            P("sp", None, "tp"),
            P("sp", "tp", None),
        ),
        out_specs=P(("sp", "tp"), None),
        check_vma=False,
    )
```

```python
import functools

import jax
import jax.numpy as jnp
from jax import lax
from jax.experimental import pallas as pl
from jax.experimental.pallas import tpu as pltpu
from jax.sharding import PartitionSpec as P

D = 2048
NOPE = 64
ROPE = 32
VH = 64
TOPK = 2
QK = 96

epsilon = 1e-06
rope_base = 10000.0
MESH_ID = pl.DeviceIdType.MESH


class Place:
    def __init__(self, n_sp, n_z):
        self.n_sp, self.n_z = n_sp, n_z
        self.sp = lax.axis_index("sp")
        self.tp = lax.axis_index("tp")
        self.core = lax.rem(self.tp, 2)
        self.z = lax.div(self.tp, 2)

    def partner(self):
        return (self.sp, self.tp + 1 - 2 * self.core)

    def sp_peer(self, step):
        return lax.rem(self.sp + step, self.n_sp)

    def z_peer(self, step):
        return lax.rem(self.z + step, self.n_z)

    def sp_id(self, index):
        return (index, self.tp)

    def z_id(self, index):
        return (self.sp, 2 * index + self.core)

    def barrier(self, use_sp, use_z):
        sem = pltpu.get_barrier_semaphore()
        count = 1
        pl.semaphore_signal(sem, inc=1, device_id=self.partner(), device_id_type=MESH_ID)
        if use_sp:
            for step in range(1, self.n_sp):
                pl.semaphore_signal(
                    sem, inc=1, device_id=self.sp_id(self.sp_peer(step)), device_id_type=MESH_ID
                )
            count += self.n_sp - 1
        if use_z:
            for step in range(1, self.n_z):
                pl.semaphore_signal(
                    sem, inc=1, device_id=self.z_id(self.z_peer(step)), device_id_type=MESH_ID
                )
            count += self.n_z - 1
        pl.semaphore_wait(sem, count)


def remote(src, dst, send, recv, device):
    return pltpu.make_async_remote_copy(
        src_ref=src,
        dst_ref=dst,
        send_sem=send,
        recv_sem=recv,
        device_id=device,
        device_id_type=MESH_ID,
    )


class GroupMove:
    def __init__(self, place, axis, scatter, x_ref, o_ref, sems):
        self.place, self.axis, self.scatter = place, axis, scatter
        self.x_ref, self.o_ref = x_ref, o_ref
        self.local_sem, self.ss, self.rs, self.ps, self.pr = sems
        self.count = place.n_sp if axis == "sp" else place.n_z
        self.me = place.sp if axis == "sp" else place.z

    def start(self):
        p, core = self.place, self.place.core
        peer, to_id = (p.sp_peer, p.sp_id) if self.axis == "sp" else (p.z_peer, p.z_id)
        own = self.x_ref.at[self.me] if self.scatter else self.x_ref
        self.copies = []
        for step in range(1, self.count):
            dst = peer(step)
            src = self.x_ref.at[dst] if self.scatter else self.x_ref
            copy = remote(
                src,
                self.o_ref.at[core, self.me],
                self.ss.at[step],
                self.rs.at[step],
                to_id(dst),
            )
            copy.start()
            self.copies.append(copy)
        self.local = pltpu.make_async_copy(own, self.o_ref.at[core, self.me], self.local_sem.at[0])
        self.local.start()
        self.relays = [
            remote(
                own, self.o_ref.at[core, self.me], self.ps.at[0], self.pr.at[0], p.partner()
            )
        ]
        self.relays[0].start()

    def relay(self):
        core = self.place.core
        for step in range(1, self.count):
            src = lax.rem(self.me - step + self.count, self.count)
            self.copies[step - 1].wait_recv()
            block = self.o_ref.at[core, src]
            copy = remote(block, block, self.ps.at[step], self.pr.at[step], self.place.partner())
            copy.start()
            self.relays.append(copy)

    def finish(self):
        for copy in self.copies:
            copy.wait_send()
        for copy in self.relays:
            copy.wait()
        self.local.wait()


def move_sems(count):
    return [pltpu.SemaphoreType.DMA((1,))] + [pltpu.SemaphoreType.DMA((count,))] * 4


def vmem():
    return pl.BlockSpec(memory_space=pltpu.VMEM)


def group_move(x, axis, scatter, n_sp, n_z, collective_id, name):
    count = n_sp if axis == "sp" else n_z
    block = x.shape[1:] if scatter else x.shape

    def kernel(x_ref, o_ref, *sems):
        place = Place(n_sp, n_z)
        place.barrier(axis == "sp", axis == "z")
        move = GroupMove(place, axis, scatter, x_ref, o_ref, sems)
        move.start()
        move.relay()
        move.finish()

    return pl.pallas_call(
        kernel,
        out_shape=jax.ShapeDtypeStruct((2, count) + block, x.dtype),
        in_specs=[vmem()],
        out_specs=vmem(),
        scratch_shapes=move_sems(count),
        compiler_params=pltpu.CompilerParams(
            collective_id=collective_id, has_side_effects=True, vmem_limit_bytes=60 << 20
        ),
        name=name,
    )(x)


def first_exchange(bundle, residual, meta, n_sp, n_z):
    def kernel(kv_ref, res_ref, meta_ref, kv_out, res_out, meta_out, kv_local, kv_s, kv_r, *sems):
        place = Place(n_sp, n_z)
        place.barrier(True, True)
        copies = []
        for step in range(1, n_sp):
            copy = remote(
                kv_ref,
                kv_out.at[place.sp],
                kv_s.at[step],
                kv_r.at[step],
                place.sp_id(place.sp_peer(step)),
            )
            copy.start()
            copies.append(copy)
        local = pltpu.make_async_copy(kv_ref, kv_out.at[place.sp], kv_local.at[0])
        local.start()
        meta_move = GroupMove(place, "z", False, meta_ref, meta_out, sems[:5])
        res_move = GroupMove(place, "z", False, res_ref, res_out, sems[5:])
        meta_move.start()
        res_move.start()
        meta_move.relay()
        res_move.relay()
        for copy in copies:
            copy.wait()
        local.wait()
        meta_move.finish()
        res_move.finish()

    return pl.pallas_call(
        kernel,
        out_shape=(
            jax.ShapeDtypeStruct((n_sp,) + bundle.shape, bundle.dtype),
            jax.ShapeDtypeStruct((2, n_z) + residual.shape, residual.dtype),
            jax.ShapeDtypeStruct((2, n_z) + meta.shape, meta.dtype),
        ),
        in_specs=[vmem()] * 3,
        out_specs=(vmem(),) * 3,
        scratch_shapes=[
            pltpu.SemaphoreType.DMA((1,)),
            pltpu.SemaphoreType.DMA((n_sp,)),
            pltpu.SemaphoreType.DMA((n_sp,)),
        ]
        + move_sems(n_z) * 2,
        compiler_params=pltpu.CompilerParams(
            collective_id=0, has_side_effects=True, vmem_limit_bytes=60 << 20
        ),
        name="first_exchange",
    )(bundle, residual, meta)


def send_rows(x, n_sp, n_z):
    rows, shared = x.shape[1], D // 4
    half = (D - shared) // 2

    def kernel(x_ref, o_ref, local_sem, *sems):
        place = Place(n_sp, n_z)
        core, me = place.core, place.sp
        place.barrier(True, True)
        side = lax.rem(place.z, 2)
        twin = place.z_id(place.z + 1 - 2 * side)
        mine = pl.ds(pl.multiple_of(shared + side * half, 128), half)
        other = pl.ds(pl.multiple_of(shared + (1 - side) * half, 128), half)
        both = pl.ds(0, shared)
        copies = []

        def push(kind, step, src, dst, device):
            copy = remote(src, dst, sems[2 * kind].at[step], sems[2 * kind + 1].at[step], device)
            copy.start()
            copies.append(copy)
            return copy

        split, direct, swapped = {}, {}, {}
        for step in range(1, n_sp):
            dst = place.sp_peer(step)
            split[step] = push(
                0, step, x_ref.at[dst, :, mine], o_ref.at[core, me, :, mine], place.sp_id(dst)
            )
        for step in range(1, n_sp):
            dst = place.sp_peer(step)
            direct[step] = push(
                1, step, x_ref.at[dst, :, both], o_ref.at[core, me, :, both], place.sp_id(dst)
            )
        local = pltpu.make_async_copy(x_ref.at[me], o_ref.at[core, me], local_sem.at[0])
        local.start()
        last = [push(3, 0, x_ref.at[me], o_ref.at[core, me], place.partner())]
        for step in range(1, n_sp):
            src = lax.rem(me - step + n_sp, n_sp)
            piece = o_ref.at[core, src, :, mine]
            split[step].wait_recv()
            swapped[step] = push(2, step, piece, piece, twin)
            last.append(push(3, step, piece, piece, place.partner()))
        for step in range(1, n_sp):
            src = lax.rem(me - step + n_sp, n_sp)
            piece = o_ref.at[core, src, :, both]
            direct[step].wait_recv()
            last.append(push(4, step, piece, piece, place.partner()))
        for step in range(1, n_sp):
            src = lax.rem(me - step + n_sp, n_sp)
            piece = o_ref.at[core, src, :, other]
            swapped[step].wait_recv()
            last.append(push(5, step, piece, piece, place.partner()))
        for copy in last:
            copy.wait_recv()
        for copy in copies:
            copy.wait_send()
        local.wait()

    return pl.pallas_call(
        kernel,
        out_shape=jax.ShapeDtypeStruct((2, n_sp, rows, D), x.dtype),
        in_specs=[vmem()],
        out_specs=vmem(),
        scratch_shapes=[pltpu.SemaphoreType.DMA((1,))] + [pltpu.SemaphoreType.DMA((n_sp,))] * 12,
        compiler_params=pltpu.CompilerParams(
            collective_id=2, has_side_effects=True, vmem_limit_bytes=60 << 20
        ),
        name="send_rows",
    )(x)


CHUNKS = 4


def return_rows(hidden, down, mixer, middle, n_sp, n_z):
    rows = hidden.shape[2]
    tok = middle.shape[0]
    width = D // CHUNKS

    def kernel(h_ref, w_ref, mix_ref, mid_ref, o_ref, ybuf, pbuf, sbuf, rbuf, cbuf, fbuf, *sems):
        pair_s, pair_r, sp_s, sp_r, z_s, z_r = sems
        place = Place(n_sp, n_z)
        core = place.core
        place.barrier(True, True)
        pairs, sends, zsends = {}, {}, {}
        order = list(range(1, n_sp)) + [0]
        for q in range(CHUNKS):
            cols = pl.ds(q * width, width)
            for step in order:
                dst = place.sp_peer(step)
                ybuf[dst, :, cols] = jnp.dot(
                    h_ref[1 - core, dst], w_ref[:, cols], preferred_element_type=jnp.float32
                ).astype(jnp.bfloat16)
                copy = remote(
                    ybuf.at[dst, :, cols],
                    pbuf.at[dst, :, cols],
                    pair_s.at[q, step],
                    pair_r.at[q, step],
                    place.partner(),
                )
                copy.start()
                pairs[q, step] = copy
        for q in range(CHUNKS):
            cols = pl.ds(q * width, width)
            for step in order:
                dst = place.sp_peer(step)
                own = jnp.dot(
                    h_ref[core, dst], w_ref[:, cols], preferred_element_type=jnp.float32
                )
                pairs[q, step].wait_recv()
                total = (own + pbuf[dst, :, cols].astype(jnp.float32)).astype(jnp.bfloat16)
                if step == 0:
                    rbuf[dst, :, cols] = total
                else:
                    sbuf[dst, :, cols] = total
                    copy = remote(
                        sbuf.at[dst, :, cols],
                        rbuf.at[place.sp, :, cols],
                        sp_s.at[q, step],
                        sp_r.at[q, step],
                        place.sp_id(dst),
                    )
                    copy.start()
                    sends[q, step] = copy
        for q in range(CHUNKS):
            cols = pl.ds(q * width, width)
            for step in range(1, n_sp):
                sends[q, step].wait_recv()
            combined = jnp.zeros((n_z * tok, width), jnp.float32)
            for src in range(n_sp):
                combined += jnp.dot(
                    mix_ref[src], rbuf[src, :, cols], preferred_element_type=jnp.float32
                )
            cbuf[:, :, cols] = combined.astype(jnp.bfloat16).reshape(n_z, tok, width)
            for step in range(1, n_z):
                dst = place.z_peer(step)
                copy = remote(
                    cbuf.at[dst, :, cols],
                    fbuf.at[place.z, :, cols],
                    z_s.at[q, step],
                    z_r.at[q, step],
                    place.z_id(dst),
                )
                copy.start()
                zsends[q, step] = copy
        for q in range(CHUNKS):
            cols = pl.ds(q * width, width)
            total = mid_ref[:, cols] + cbuf[place.z, :, cols].astype(jnp.float32)
            for step in range(1, n_z):
                src = lax.rem(place.z - step + n_z, n_z)
                zsends[q, step].wait_recv()
                total += fbuf[src, :, cols].astype(jnp.float32)
            o_ref[:, cols] = total.astype(jnp.bfloat16)
        for group in (pairs, sends, zsends):
            for copy in group.values():
                copy.wait_send()

    dma = pltpu.SemaphoreType.DMA
    block = pltpu.VMEM((n_sp, rows, D), jnp.bfloat16)
    zblock = pltpu.VMEM((n_z, tok, D), jnp.bfloat16)
    return pl.pallas_call(
        kernel,
        out_shape=jax.ShapeDtypeStruct((tok, D), jnp.bfloat16),
        in_specs=[vmem()] * 4,
        out_specs=vmem(),
        scratch_shapes=[block, block, block, block, zblock, zblock]
        + [dma((CHUNKS, n_sp))] * 4
        + [dma((CHUNKS, n_z))] * 2,
        compiler_params=pltpu.CompilerParams(
            collective_id=3, has_side_effects=True, vmem_limit_bytes=60 << 20
        ),
        name="return_rows",
    )(hidden, down, mixer, middle)


def rms_scale(values):
    return lax.rsqrt(jnp.mean(values * values, axis=-1, keepdims=True) + epsilon)


def rotate_half(values, angles):
    half_dims = values.shape[-1] // 2
    first_half = values[..., :half_dims]
    second_half = values[..., half_dims:]
    cosine = jnp.cos(angles)
    sine_val = jnp.sin(angles)
    return jnp.concatenate(
        [
            first_half * cosine - second_half * sine_val,
            second_half * cosine + first_half * sine_val,
        ],
        axis=-1,
    )


def head_prepare(raw_rows, gain_vec, angles):
    normed_rows = raw_rows * rms_scale(raw_rows) * gain_vec
    turned_rows = rotate_half(normed_rows[..., NOPE:], angles[:, None, :])
    return jnp.concatenate([normed_rows[..., :NOPE], turned_rows], axis=-1).astype(jnp.bfloat16)


def shards(
    queries,
    latent,
    rot_key,
    latent_gain,
    key_up,
    value_up,
    query_gain,
    key_gain,
    out_gain,
    out_weight,
    residual,
    ffn_gain,
    routes,
    route_weights,
    expert_gate,
    expert_up,
    expert_down,
):
    shard_len = queries.shape[0]
    local_heads = key_up.shape[1] // NOPE
    sp_count = lax.axis_size("sp")
    tp_count = lax.axis_size("tp")
    z_count = tp_count // 2
    tok_count = residual.shape[0]
    my_first = lax.axis_index("sp") * shard_len
    my_last = my_first + shard_len - 1
    positions = my_first + jnp.arange(shard_len, dtype=jnp.int32)
    inverse = rope_base ** (-jnp.arange(0, ROPE, 2, dtype=jnp.float32) / ROPE)
    angles = positions.astype(jnp.float32)[:, None] * inverse[None, :]
    lat_f32 = latent.astype(jnp.float32)
    normed_latent = (lat_f32 * rms_scale(lat_f32) * latent_gain).astype(jnp.bfloat16)
    key_nope = jnp.dot(normed_latent, key_up, preferred_element_type=jnp.float32).astype(
        jnp.bfloat16
    )
    value_rows = jnp.dot(normed_latent, value_up, preferred_element_type=jnp.float32).astype(
        jnp.bfloat16
    )
    shared = jnp.broadcast_to(
        rot_key.astype(jnp.float32)[:, None, :], (shard_len, local_heads, ROPE)
    )
    raw_keys = jnp.concatenate(
        [key_nope.astype(jnp.float32).reshape(shard_len, local_heads, NOPE), shared], axis=-1
    )
    key_rows = head_prepare(raw_keys, key_gain, angles)
    query_rows = head_prepare(
        queries.astype(jnp.float32).reshape(shard_len, local_heads, QK), query_gain, angles
    )
    query_heads = jnp.transpose(query_rows, (1, 0, 2))
    bundle = jnp.concatenate(
        [
            jnp.transpose(key_rows, (1, 2, 0)),
            jnp.transpose(value_rows.reshape(shard_len, local_heads, VH), (1, 2, 0)),
        ],
        axis=1,
    )
    score_scale = QK ** (-0.5)
    init_state = (
        jnp.full((local_heads, shard_len), -1e30, jnp.float32),
        jnp.zeros((local_heads, shard_len), jnp.float32),
        jnp.zeros((local_heads, shard_len, VH), jnp.float32),
    )
    meta = jnp.concatenate(
        [
            routes.astype(jnp.float32),
            route_weights,
            jnp.zeros((tok_count, 128 - 2 * TOPK), jnp.float32),
        ],
        axis=1,
    )
    key_piece, residual_all, meta_all = first_exchange(bundle, residual, meta, sp_count, z_count)
    block_count = sp_count

    def one_block(block_index, running_state):
        first_key = block_index * shard_len

        def compute(inner):
            row_peak, row_total, weighted = inner
            key_part = lax.dynamic_index_in_dim(key_piece, block_index, 0, keepdims=False)
            scores = (
                jnp.einsum(
                    "hqc,hck->hqk",
                    query_heads,
                    key_part[:, :QK, :],
                    preferred_element_type=jnp.float32,
                )
                * score_scale
            )
            key_pos = first_key + jnp.arange(shard_len, dtype=jnp.int32)
            allowed = key_pos[None, None, :] <= positions[None, :, None]
            scores = jnp.where(allowed, scores, -1e30)
            new_peak = jnp.maximum(row_peak, jnp.max(scores, axis=2))
            exponent = jnp.where(allowed, jnp.exp(scores - new_peak[..., None]), 0.0)
            factor = jnp.exp(row_peak - new_peak)
            new_total = row_total * factor + jnp.sum(exponent, axis=2)
            contrib = jnp.einsum(
                "hqk,hvk->hqv",
                exponent.astype(jnp.bfloat16),
                key_part[:, QK:, :],
                preferred_element_type=jnp.float32,
            )
            return (new_peak, new_total, weighted * factor[..., None] + contrib)

        return lax.cond(first_key <= my_last, compute, lambda inner: inner, running_state)

    row_peak, row_total, weighted = lax.fori_loop(0, block_count, one_block, init_state)
    attended = (weighted / row_total[..., None]).astype(jnp.bfloat16)
    head_major = jnp.transpose(attended, (1, 0, 2)).reshape(shard_len, local_heads * VH)
    gathered = group_move(head_major, "z", False, sp_count, z_count, 1, "gather_heads")
    att_rows = (
        jnp.transpose(gathered, (2, 1, 0, 3)).reshape(shard_len, -1).astype(jnp.float32)
    )
    normed_rows = (att_rows * rms_scale(att_rows) * out_gain).astype(jnp.bfloat16)
    mixed = jnp.dot(normed_rows, out_weight, preferred_element_type=jnp.float32)
    residual_rows = jnp.transpose(residual_all, (1, 0, 2, 3)).reshape(shard_len, D)
    middle = residual_rows.astype(jnp.float32) + mixed
    ffn_input = (middle * rms_scale(middle) * ffn_gain).astype(jnp.bfloat16)
    own_middle = lax.dynamic_slice_in_dim(
        middle, lax.axis_index("tp") * tok_count, tok_count, 0
    )
    slot_cap = max(2, 9 * tok_count * TOPK // (8 * sp_count))
    rows = z_count * slot_cap
    core = lax.axis_index("tp") % 2
    part_meta = lax.dynamic_index_in_dim(meta_all, core, 0, keepdims=False)
    part_routes = part_meta[:, :, :TOPK].astype(jnp.int32).reshape(z_count, tok_count * TOPK)
    part_weights = part_meta[:, :, TOPK : 2 * TOPK].reshape(z_count * tok_count, TOPK)
    one_hot = (part_routes[:, :, None] == jnp.arange(sp_count, dtype=jnp.int32)).astype(jnp.int32)
    earlier = jnp.cumsum(one_hot, axis=1) - one_hot
    rank_in = jnp.sum(earlier * one_hot, axis=2)
    slots = rank_in + jnp.arange(z_count, dtype=jnp.int32)[:, None] * slot_cap
    targets = (part_routes * rows + slots).reshape(z_count * tok_count, TOPK)
    hits = targets[:, :, None] == jnp.arange(sp_count * rows, dtype=jnp.int32)
    chooser = jnp.sum(hits.astype(jnp.bfloat16), axis=1)
    mixer = jnp.sum(jnp.where(hits, part_weights[:, :, None], 0.0), axis=1).astype(jnp.bfloat16)
    mixer = jnp.transpose(mixer.reshape(z_count * tok_count, sp_count, rows), (1, 0, 2))
    part_input = lax.dynamic_index_in_dim(
        ffn_input.reshape(z_count, 2, tok_count, D), core, 1, keepdims=False
    ).reshape(z_count * tok_count, D)
    outbound = (
        jnp.einsum("ts,td->sd", chooser, part_input, preferred_element_type=jnp.float32)
        .astype(jnp.bfloat16)
        .reshape(sp_count, rows, D)
    )
    arrived = send_rows(outbound, sp_count, z_count)
    row_block = arrived.reshape(2 * sp_count * rows, D)
    gate_pre = jnp.dot(row_block, expert_gate[0], preferred_element_type=jnp.float32)
    up_pre = jnp.dot(row_block, expert_up[0], preferred_element_type=jnp.float32)
    hidden = (jax.nn.silu(gate_pre) * up_pre).astype(jnp.bfloat16)
    return return_rows(
        hidden.reshape(2, sp_count, rows, -1),
        expert_down[0],
        mixer,
        own_middle,
        sp_count,
        z_count,
    )


def solution(mesh):
    return jax.shard_map(
        shards,
        mesh=mesh,
        in_specs=(
            P("sp", "tp"),
            P("sp", None),
            P("sp", None),
            P(),
            P(None, "tp"),
            P(None, "tp"),
            P(),
            P(),
            P(),
            P(),
            P(("sp", "tp"), None),
            P(),
            P(("sp", "tp"), None),
            P(("sp", "tp"), None),
            P("sp", None, "tp"),
            P("sp", None, "tp"),
            P("sp", "tp", None),
        ),
        out_specs=P(("sp", "tp"), None),
        check_vma=False,
    )
```

```python
import functools

import jax
import jax.numpy as jnp
from jax import lax
from jax.experimental import pallas as pl
from jax.experimental.pallas import tpu as pltpu
from jax.sharding import PartitionSpec as P

D = 2048
NOPE = 64
ROPE = 32
VH = 64
TOPK = 2
QK = 96

epsilon = 1e-06
rope_base = 10000.0
MESH_ID = pl.DeviceIdType.MESH


class Place:
    def __init__(self, n_sp, n_z):
        self.n_sp, self.n_z = n_sp, n_z
        self.sp = lax.axis_index("sp")
        self.tp = lax.axis_index("tp")
        self.core = lax.rem(self.tp, 2)
        self.z = lax.div(self.tp, 2)

    def partner(self):
        return (self.sp, self.tp + 1 - 2 * self.core)

    def sp_peer(self, step):
        return lax.rem(self.sp + step, self.n_sp)

    def z_peer(self, step):
        return lax.rem(self.z + step, self.n_z)

    def sp_id(self, index):
        return (index, self.tp)

    def z_id(self, index):
        return (self.sp, 2 * index + self.core)

    def barrier(self, use_sp, use_z):
        sem = pltpu.get_barrier_semaphore()
        count = 1
        pl.semaphore_signal(sem, inc=1, device_id=self.partner(), device_id_type=MESH_ID)
        if use_sp:
            for step in range(1, self.n_sp):
                pl.semaphore_signal(
                    sem, inc=1, device_id=self.sp_id(self.sp_peer(step)), device_id_type=MESH_ID
                )
            count += self.n_sp - 1
        if use_z:
            for step in range(1, self.n_z):
                pl.semaphore_signal(
                    sem, inc=1, device_id=self.z_id(self.z_peer(step)), device_id_type=MESH_ID
                )
            count += self.n_z - 1
        pl.semaphore_wait(sem, count)


def remote(src, dst, send, recv, device):
    return pltpu.make_async_remote_copy(
        src_ref=src,
        dst_ref=dst,
        send_sem=send,
        recv_sem=recv,
        device_id=device,
        device_id_type=MESH_ID,
    )


def vmem():
    return pl.BlockSpec(memory_space=pltpu.VMEM)


def gather_heads(x, n_sp, n_z):
    n_tp = 2 * n_z

    def kernel(x_ref, o_ref, local_sem, send_sem, recv_sem):
        place = Place(n_sp, n_z)
        sem = pltpu.get_barrier_semaphore()
        for step in range(1, n_tp):
            pl.semaphore_signal(
                sem,
                inc=1,
                device_id=(place.sp, lax.rem(place.tp + step, n_tp)),
                device_id_type=MESH_ID,
            )
        pl.semaphore_wait(sem, n_tp - 1)
        copies = []
        for step in range(1, n_tp):
            dst = lax.rem(place.tp + step, n_tp)
            copy = remote(
                x_ref.at[lax.rem(dst, 2)],
                o_ref.at[place.tp],
                send_sem.at[step],
                recv_sem.at[step],
                (place.sp, dst),
            )
            copy.start()
            copies.append(copy)
        local = pltpu.make_async_copy(x_ref.at[place.core], o_ref.at[place.tp], local_sem.at[0])
        local.start()
        for copy in copies:
            copy.wait()
        local.wait()

    return pl.pallas_call(
        kernel,
        out_shape=jax.ShapeDtypeStruct((n_tp,) + x.shape[1:], x.dtype),
        in_specs=[vmem()],
        out_specs=vmem(),
        scratch_shapes=[
            pltpu.SemaphoreType.DMA((1,)),
            pltpu.SemaphoreType.DMA((n_tp,)),
            pltpu.SemaphoreType.DMA((n_tp,)),
        ],
        compiler_params=pltpu.CompilerParams(
            collective_id=1, has_side_effects=True, vmem_limit_bytes=60 << 20
        ),
        name="gather_heads",
    )(x)


def first_exchange(bundle, residual, meta, n_sp, n_z):
    def kernel(kv_ref, res_ref, meta_ref, kv_out, res_out, meta_out, local_sem, *sems):
        place = Place(n_sp, n_z)
        place.barrier(True, True)
        moves = (
            (meta_ref, meta_out, n_z, place.z, place.z_peer, place.z_id),
            (res_ref, res_out, n_z, place.z, place.z_peer, place.z_id),
            (kv_ref, kv_out, n_sp, place.sp, place.sp_peer, place.sp_id),
        )
        copies = []
        for number, (src, out, count, me, peer, to_id) in enumerate(moves):
            for step in range(1, count):
                copy = remote(
                    src,
                    out.at[me],
                    sems[2 * number].at[step],
                    sems[2 * number + 1].at[step],
                    to_id(peer(step)),
                )
                copy.start()
                copies.append(copy)
            local = pltpu.make_async_copy(src, out.at[me], local_sem.at[number])
            local.start()
            copies.append(local)
        for copy in copies:
            copy.wait()

    dma = pltpu.SemaphoreType.DMA
    return pl.pallas_call(
        kernel,
        out_shape=(
            jax.ShapeDtypeStruct((n_sp,) + bundle.shape, bundle.dtype),
            jax.ShapeDtypeStruct((n_z,) + residual.shape, residual.dtype),
            jax.ShapeDtypeStruct((n_z,) + meta.shape, meta.dtype),
        ),
        in_specs=[vmem()] * 3,
        out_specs=(vmem(),) * 3,
        scratch_shapes=[dma((3,))] + [dma((n_z,))] * 4 + [dma((n_sp,))] * 2,
        compiler_params=pltpu.CompilerParams(
            collective_id=0, has_side_effects=True, vmem_limit_bytes=60 << 20
        ),
        name="first_exchange",
    )(bundle, residual, meta)


def send_rows(x, n_sp, n_z):
    rows, shared = x.shape[1], D // 4
    half = (D - shared) // 2

    def kernel(x_ref, o_ref, local_sem, *sems):
        place = Place(n_sp, n_z)
        core, me = place.core, place.sp
        place.barrier(True, True)
        side = lax.rem(place.z, 2)
        twin = place.z_id(place.z + 1 - 2 * side)
        mine = pl.ds(pl.multiple_of(shared + side * half, 128), half)
        other = pl.ds(pl.multiple_of(shared + (1 - side) * half, 128), half)
        both = pl.ds(0, shared)
        copies = []

        def push(kind, step, src, dst, device):
            copy = remote(src, dst, sems[2 * kind].at[step], sems[2 * kind + 1].at[step], device)
            copy.start()
            copies.append(copy)
            return copy

        split, direct, swapped = {}, {}, {}
        for step in range(1, n_sp):
            dst = place.sp_peer(step)
            split[step] = push(
                0, step, x_ref.at[dst, :, mine], o_ref.at[core, me, :, mine], place.sp_id(dst)
            )
        for step in range(1, n_sp):
            dst = place.sp_peer(step)
            direct[step] = push(
                1, step, x_ref.at[dst, :, both], o_ref.at[core, me, :, both], place.sp_id(dst)
            )
        local = pltpu.make_async_copy(x_ref.at[me], o_ref.at[core, me], local_sem.at[0])
        local.start()
        last = [push(3, 0, x_ref.at[me], o_ref.at[core, me], place.partner())]
        for step in range(1, n_sp):
            src = lax.rem(me - step + n_sp, n_sp)
            piece = o_ref.at[core, src, :, mine]
            split[step].wait_recv()
            swapped[step] = push(2, step, piece, piece, twin)
            last.append(push(3, step, piece, piece, place.partner()))
        for step in range(1, n_sp):
            src = lax.rem(me - step + n_sp, n_sp)
            piece = o_ref.at[core, src, :, both]
            direct[step].wait_recv()
            last.append(push(4, step, piece, piece, place.partner()))
        for step in range(1, n_sp):
            src = lax.rem(me - step + n_sp, n_sp)
            piece = o_ref.at[core, src, :, other]
            swapped[step].wait_recv()
            last.append(push(5, step, piece, piece, place.partner()))
        for copy in last:
            copy.wait_recv()
        for copy in copies:
            copy.wait_send()
        local.wait()

    return pl.pallas_call(
        kernel,
        out_shape=jax.ShapeDtypeStruct((2, n_sp, rows, D), x.dtype),
        in_specs=[vmem()],
        out_specs=vmem(),
        scratch_shapes=[pltpu.SemaphoreType.DMA((1,))] + [pltpu.SemaphoreType.DMA((n_sp,))] * 12,
        compiler_params=pltpu.CompilerParams(
            collective_id=2, has_side_effects=True, vmem_limit_bytes=60 << 20
        ),
        name="send_rows",
    )(x)


CHUNKS = 4


def return_rows(hidden, down, mixer, middle, n_sp, n_z):
    rows = hidden.shape[2]
    tok = middle.shape[0]
    width = D // CHUNKS

    def kernel(h_ref, w_ref, mix_ref, mid_ref, o_ref, ybuf, pbuf, sbuf, rbuf, cbuf, fbuf, *sems):
        pair_s, pair_r, sp_s, sp_r, z_s, z_r = sems
        place = Place(n_sp, n_z)
        core = place.core
        place.barrier(True, True)
        pairs, sends, zsends = {}, {}, {}
        order = list(range(1, n_sp)) + [0]
        for q in range(CHUNKS):
            cols = pl.ds(q * width, width)
            for step in order:
                dst = place.sp_peer(step)
                ybuf[dst, :, cols] = jnp.dot(
                    h_ref[1 - core, dst], w_ref[:, cols], preferred_element_type=jnp.float32
                ).astype(jnp.bfloat16)
                copy = remote(
                    ybuf.at[dst, :, cols],
                    pbuf.at[dst, :, cols],
                    pair_s.at[q, step],
                    pair_r.at[q, step],
                    place.partner(),
                )
                copy.start()
                pairs[q, step] = copy
        for q in range(CHUNKS):
            cols = pl.ds(q * width, width)
            for step in order:
                dst = place.sp_peer(step)
                own = jnp.dot(
                    h_ref[core, dst], w_ref[:, cols], preferred_element_type=jnp.float32
                )
                pairs[q, step].wait_recv()
                total = (own + pbuf[dst, :, cols].astype(jnp.float32)).astype(jnp.bfloat16)
                if step == 0:
                    rbuf[dst, :, cols] = total
                else:
                    sbuf[dst, :, cols] = total
                    copy = remote(
                        sbuf.at[dst, :, cols],
                        rbuf.at[place.sp, :, cols],
                        sp_s.at[q, step],
                        sp_r.at[q, step],
                        place.sp_id(dst),
                    )
                    copy.start()
                    sends[q, step] = copy
        for q in range(CHUNKS):
            cols = pl.ds(q * width, width)
            for step in range(1, n_sp):
                sends[q, step].wait_recv()
            combined = jnp.zeros((n_z * tok, width), jnp.float32)
            for src in range(n_sp):
                combined += jnp.dot(
                    mix_ref[src], rbuf[src, :, cols], preferred_element_type=jnp.float32
                )
            cbuf[:, :, cols] = combined.astype(jnp.bfloat16).reshape(n_z, tok, width)
            for step in range(1, n_z):
                dst = place.z_peer(step)
                copy = remote(
                    cbuf.at[dst, :, cols],
                    fbuf.at[place.z, :, cols],
                    z_s.at[q, step],
                    z_r.at[q, step],
                    place.z_id(dst),
                )
                copy.start()
                zsends[q, step] = copy
        for q in range(CHUNKS):
            cols = pl.ds(q * width, width)
            total = mid_ref[:, cols] + cbuf[place.z, :, cols].astype(jnp.float32)
            for step in range(1, n_z):
                src = lax.rem(place.z - step + n_z, n_z)
                zsends[q, step].wait_recv()
                total += fbuf[src, :, cols].astype(jnp.float32)
            o_ref[:, cols] = total.astype(jnp.bfloat16)
        for group in (pairs, sends, zsends):
            for copy in group.values():
                copy.wait_send()

    dma = pltpu.SemaphoreType.DMA
    block = pltpu.VMEM((n_sp, rows, D), jnp.bfloat16)
    zblock = pltpu.VMEM((n_z, tok, D), jnp.bfloat16)
    return pl.pallas_call(
        kernel,
        out_shape=jax.ShapeDtypeStruct((tok, D), jnp.bfloat16),
        in_specs=[vmem()] * 4,
        out_specs=vmem(),
        scratch_shapes=[block, block, block, block, zblock, zblock]
        + [dma((CHUNKS, n_sp))] * 4
        + [dma((CHUNKS, n_z))] * 2,
        compiler_params=pltpu.CompilerParams(
            collective_id=3, has_side_effects=True, vmem_limit_bytes=60 << 20
        ),
        name="return_rows",
    )(hidden, down, mixer, middle)


def rms_scale(values):
    return lax.rsqrt(jnp.mean(values * values, axis=-1, keepdims=True) + epsilon)


def rotate_half(values, angles):
    half_dims = values.shape[-1] // 2
    first_half = values[..., :half_dims]
    second_half = values[..., half_dims:]
    cosine = jnp.cos(angles)
    sine_val = jnp.sin(angles)
    return jnp.concatenate(
        [
            first_half * cosine - second_half * sine_val,
            second_half * cosine + first_half * sine_val,
        ],
        axis=-1,
    )


def head_prepare(raw_rows, gain_vec, angles):
    normed_rows = raw_rows * rms_scale(raw_rows) * gain_vec
    turned_rows = rotate_half(normed_rows[..., NOPE:], angles[:, None, :])
    return jnp.concatenate([normed_rows[..., :NOPE], turned_rows], axis=-1).astype(jnp.bfloat16)


def shards(
    queries,
    latent,
    rot_key,
    latent_gain,
    key_up,
    value_up,
    query_gain,
    key_gain,
    out_gain,
    out_weight,
    residual,
    ffn_gain,
    routes,
    route_weights,
    expert_gate,
    expert_up,
    expert_down,
):
    shard_len = queries.shape[0]
    local_heads = key_up.shape[1] // NOPE
    sp_count = lax.axis_size("sp")
    tp_count = lax.axis_size("tp")
    z_count = tp_count // 2
    tok_count = residual.shape[0]
    my_first = lax.axis_index("sp") * shard_len
    my_last = my_first + shard_len - 1
    positions = my_first + jnp.arange(shard_len, dtype=jnp.int32)
    inverse = rope_base ** (-jnp.arange(0, ROPE, 2, dtype=jnp.float32) / ROPE)
    angles = positions.astype(jnp.float32)[:, None] * inverse[None, :]
    lat_f32 = latent.astype(jnp.float32)
    normed_latent = (lat_f32 * rms_scale(lat_f32) * latent_gain).astype(jnp.bfloat16)
    key_nope = jnp.dot(normed_latent, key_up, preferred_element_type=jnp.float32).astype(
        jnp.bfloat16
    )
    value_rows = jnp.dot(normed_latent, value_up, preferred_element_type=jnp.float32).astype(
        jnp.bfloat16
    )
    shared = jnp.broadcast_to(
        rot_key.astype(jnp.float32)[:, None, :], (shard_len, local_heads, ROPE)
    )
    raw_keys = jnp.concatenate(
        [key_nope.astype(jnp.float32).reshape(shard_len, local_heads, NOPE), shared], axis=-1
    )
    key_rows = head_prepare(raw_keys, key_gain, angles)
    query_rows = head_prepare(
        queries.astype(jnp.float32).reshape(shard_len, local_heads, QK), query_gain, angles
    )
    query_heads = jnp.transpose(query_rows, (1, 0, 2))
    bundle = jnp.concatenate(
        [
            jnp.transpose(key_rows, (1, 2, 0)),
            jnp.transpose(value_rows.reshape(shard_len, local_heads, VH), (1, 2, 0)),
        ],
        axis=1,
    )
    score_scale = QK ** (-0.5)
    init_state = (
        jnp.full((local_heads, shard_len), -1e30, jnp.float32),
        jnp.zeros((local_heads, shard_len), jnp.float32),
        jnp.zeros((local_heads, shard_len, VH), jnp.float32),
    )
    meta = jnp.concatenate(
        [
            routes.astype(jnp.float32),
            route_weights,
            jnp.zeros((tok_count, 128 - 2 * TOPK), jnp.float32),
        ],
        axis=1,
    )
    key_piece, residual_all, meta_all = first_exchange(bundle, residual, meta, sp_count, z_count)
    block_count = sp_count

    def one_block(block_index, running_state):
        first_key = block_index * shard_len

        def compute(inner):
            row_peak, row_total, weighted = inner
            key_part = lax.dynamic_index_in_dim(key_piece, block_index, 0, keepdims=False)
            scores = (
                jnp.einsum(
                    "hqc,hck->hqk",
                    query_heads,
                    key_part[:, :QK, :],
                    preferred_element_type=jnp.float32,
                )
                * score_scale
            )
            key_pos = first_key + jnp.arange(shard_len, dtype=jnp.int32)
            allowed = key_pos[None, None, :] <= positions[None, :, None]
            scores = jnp.where(allowed, scores, -1e30)
            new_peak = jnp.maximum(row_peak, jnp.max(scores, axis=2))
            exponent = jnp.where(allowed, jnp.exp(scores - new_peak[..., None]), 0.0)
            factor = jnp.exp(row_peak - new_peak)
            new_total = row_total * factor + jnp.sum(exponent, axis=2)
            contrib = jnp.einsum(
                "hqk,hvk->hqv",
                exponent.astype(jnp.bfloat16),
                key_part[:, QK:, :],
                preferred_element_type=jnp.float32,
            )
            return (new_peak, new_total, weighted * factor[..., None] + contrib)

        return lax.cond(first_key <= my_last, compute, lambda inner: inner, running_state)

    row_peak, row_total, weighted = lax.fori_loop(0, block_count, one_block, init_state)
    attended = (weighted / row_total[..., None]).astype(jnp.bfloat16)
    part_len = z_count * tok_count
    by_core = (
        attended.reshape(local_heads, z_count, 2, tok_count, VH)
        .transpose(2, 1, 3, 0, 4)
        .reshape(2, part_len, local_heads * VH)
    )
    gathered = gather_heads(by_core, sp_count, z_count)
    att_rows = jnp.transpose(gathered, (1, 0, 2)).reshape(part_len, -1).astype(jnp.float32)
    normed_rows = (att_rows * rms_scale(att_rows) * out_gain).astype(jnp.bfloat16)
    mixed = jnp.dot(normed_rows, out_weight, preferred_element_type=jnp.float32)
    middle = residual_all.reshape(part_len, D).astype(jnp.float32) + mixed
    part_input = (middle * rms_scale(middle) * ffn_gain).astype(jnp.bfloat16)
    own_middle = lax.dynamic_slice_in_dim(
        middle, lax.axis_index("tp") // 2 * tok_count, tok_count, 0
    )
    slot_cap = max(2, 9 * tok_count * TOPK // (8 * sp_count))
    rows = z_count * slot_cap
    part_routes = meta_all[:, :, :TOPK].astype(jnp.int32).reshape(z_count, tok_count * TOPK)
    part_weights = meta_all[:, :, TOPK : 2 * TOPK].reshape(z_count * tok_count, TOPK)
    one_hot = (part_routes[:, :, None] == jnp.arange(sp_count, dtype=jnp.int32)).astype(jnp.int32)
    earlier = jnp.cumsum(one_hot, axis=1) - one_hot
    rank_in = jnp.sum(earlier * one_hot, axis=2)
    slots = rank_in + jnp.arange(z_count, dtype=jnp.int32)[:, None] * slot_cap
    targets = (part_routes * rows + slots).reshape(z_count * tok_count, TOPK)
    hits = targets[:, :, None] == jnp.arange(sp_count * rows, dtype=jnp.int32)
    chooser = jnp.sum(hits.astype(jnp.bfloat16), axis=1)
    mixer = jnp.sum(jnp.where(hits, part_weights[:, :, None], 0.0), axis=1).astype(jnp.bfloat16)
    mixer = jnp.transpose(mixer.reshape(z_count * tok_count, sp_count, rows), (1, 0, 2))
    outbound = (
        jnp.einsum("ts,td->sd", chooser, part_input, preferred_element_type=jnp.float32)
        .astype(jnp.bfloat16)
        .reshape(sp_count, rows, D)
    )
    arrived = send_rows(outbound, sp_count, z_count)
    row_block = arrived.reshape(2 * sp_count * rows, D)
    gate_pre = jnp.dot(row_block, expert_gate[0], preferred_element_type=jnp.float32)
    up_pre = jnp.dot(row_block, expert_up[0], preferred_element_type=jnp.float32)
    hidden = (jax.nn.silu(gate_pre) * up_pre).astype(jnp.bfloat16)
    return return_rows(
        hidden.reshape(2, sp_count, rows, -1),
        expert_down[0],
        mixer,
        own_middle,
        sp_count,
        z_count,
    )


def solution(mesh):
    return jax.shard_map(
        shards,
        mesh=mesh,
        in_specs=(
            P("sp", "tp"),
            P("sp", None),
            P("sp", None),
            P(),
            P(None, "tp"),
            P(None, "tp"),
            P(),
            P(),
            P(),
            P(),
            P(("sp", "tp"), None),
            P(),
            P(("sp", "tp"), None),
            P(("sp", "tp"), None),
            P("sp", None, "tp"),
            P("sp", None, "tp"),
            P("sp", "tp", None),
        ),
        out_specs=P(("sp", "tp"), None),
        check_vma=False,
    )
```
